32 devices in a mesh: ep: 4 (over y, x), tp: 8 (over z, core).
Axes of the slice: x: 2, y: 2, z: 4, core: 2. Of those that a mesh axis runs over, the one named last changes fastest.
Arguments:
- queries: bfloat16 [4096, 2048], P('ep', 'tp'), may hold values from -200 to 200
- key_rows: bfloat16 [4096, 1024], P('ep', 'tp'), may hold values from -6 to 6
- value_rows: bfloat16 [4096, 1024], P('ep', 'tp'), may hold values from -24 to 24
- sink_logits: float32 [32], P('tp'), may hold values from 2 to 6
- out_weight: bfloat16 [2048, 2048], P('tp'), may hold values from -0.125 to 0.125
- expert_input: bfloat16 [3072, 2048], P(('ep', 'tp')), may hold values from -6 to 6
- norm_gain: float32 [2048], replicated, may hold values from 0.1 to 1.9
- group_ids: int32 [3072, 1], P(('ep', 'tp')), may hold values from 0 to 3; in each aligned block of 96 rows (0 to 95, 96 to 191, ...) at most 30 rows name the same one
- route_weight: float32 [3072, 2], P(('ep', 'tp')), may hold values from 0.2 to 1
- gate_weight: bfloat16 [8, 2048, 4096], P('ep', None, 'tp'), may hold values from -0.125 to 0.125
- up_weight: bfloat16 [8, 2048, 4096], P('ep', None, 'tp'), may hold values from -0.125 to 0.125
- down_weight: bfloat16 [8, 4096, 2048], P('ep', 'tp'), may hold values from -0.09375 to 0.09375
Outputs:
- attn_output: bfloat16 [4096, 2048], P(('ep', 'tp'))
- expert_output: bfloat16 [3072, 2048], P(('ep', 'tp'))
The draws below stay inside these ranges and needn't reach their ends.
Inputs may be any that keep to these rules, and one draw needn't show every extreme that they name: `group_ids`: in the rows of one device (aligned blocks of 96 rows), no group is named by more than 30 rows, and in every draw some group is named by exactly 30 rows of some block.
All inputs are finite; a program needn't handle non-finite values.
Results may differ from the reference program's by a relative error of at most 0.02.
Values may be sent and summed in bfloat16 or wider, within the bound.
No kernel may reach another device: no remote copies, remote signals or barrier semaphores. Data moves between devices by JAX's collectives and lax.ppermute only.
A program may use at most 128 MiB of HBM per device.

```python
import math
import jax
import jax.numpy as jnp
import numpy as np
from jax import lax

D = 2048
HD = 64
HEADS = 32
KV_HEADS = 16
WINDOW = 128
DE = 4096
EXP_DEV = 2
TB = 96
EXPERTS = 8
CAP = 30
TOK_A = 4096
TOK_B = 3072
N_EP = 4
N_TP = 8


def drawn_keys(key):
    base_keys = jax.random.normal(jax.random.fold_in(key, 11), (TOK_A, KV_HEADS, HD), jnp.float32)
    return jnp.clip(base_keys, -6.0, 6.0)


def draw_key_rows(key, part):
    return drawn_keys(key).reshape(TOK_A, KV_HEADS * HD).astype(jnp.bfloat16)


def draw_queries(key, part):
    fresh = jax.random.normal(jax.random.fold_in(key, 21), (TOK_A, HEADS, HD), jnp.float32)
    fresh = jnp.clip(fresh, -6.0, 6.0)
    return fresh.reshape(TOK_A, HEADS * HD).astype(jnp.bfloat16)


def block_scale(stream_key, dims, shards, smallest, top_value):
    def one(dim, blocks):
        draws = jax.random.uniform(jax.random.fold_in(jax.random.fold_in(stream_key, 6), dim), (blocks,), jnp.float32, smallest / len(shards), top_value / len(shards))
        return jnp.repeat(jnp.exp(draws), dims[dim] // blocks).reshape((-1,) + (1,) * (len(dims) - dim - 1))

    gain = one(*shards[0])
    for cut in shards[1:]:
        gain = gain * one(*cut)
    return gain


def routed_block(own_key, own, number, rows, count, top, reach, slope):
    sequence = jax.random.permutation(own_key, count)
    crowded, common = load_shares(count, rows * top, reach, slope, True), load_shares(count, rows * top, reach, slope, False)
    places = jnp.arange(count)

    def named(lengths, rotation):
        used = int((lengths > 0).sum())
        fixed = max(1, used // 4)
        passed = fixed + (places - fixed + rotation * (used - fixed)) % max(1, count - fixed)
        return jnp.zeros((count,), jnp.int32).at[sequence[jnp.where(places < fixed, places, passed)]].set(jnp.asarray(lengths, jnp.int32))

    lengths = jnp.where(number % 4 == 0, named(crowded, number // 4), named(common, number - number // 4 - 1))
    mixed = jax.random.permutation(jax.random.fold_in(own, 3), count)
    donor, sink = mixed[0:count // 2 * 2:2], mixed[1:count // 2 * 2:2]
    slack = jnp.minimum(lengths[donor] - 1, reach - lengths[sink]) // 2
    slack = jnp.where((donor == sequence[0]) | (sink == sequence[0]) | (lengths[sink] == 0), 0, jnp.maximum(slack, 0))
    passed = jax.random.randint(jax.random.fold_in(own, 4), (count // 2,), 0, 1 << 20) % (slack + 1)
    lengths = lengths.at[donor].add(-passed).at[sink].add(passed)
    labels = jnp.searchsorted(jnp.cumsum(lengths), jnp.arange(rows * top), side="right").astype(jnp.int32)
    table = labels.reshape(top, rows).T
    table = table[jax.random.permutation(jax.random.fold_in(own, 1), rows)]
    rotation = jax.random.randint(jax.random.fold_in(own, 2), (rows, 1), 0, top)
    return jnp.take_along_axis(table, (jnp.arange(top)[None, :] + rotation) % top, axis=1)


def load_shares(number_of, total, reach, skew, full):
    loads = [(1 << 20) // math.isqrt(standing ** skew) + 1 for standing in range(1, number_of + 1)]
    largest = reach if full else min(reach, max(-(-total // number_of), total * loads[0] // sum(loads)))
    least = 1 if total - largest >= number_of - 1 else 0
    holding, spare = [largest] + [least] * (number_of - 1), total - largest - least * (number_of - 1)
    while spare > 0:
        free = [i for i in range(1, number_of) if holding[i] < largest] or [i for i in range(1, number_of) if holding[i] < reach]
        whole, remaining = sum([loads[i] for i in free]), spare
        for i in free:
            extra = min(reach - holding[i], max(1, remaining * loads[i] // whole), spare)
            holding[i] = holding[i] + extra
            spare = spare - extra
    return np.array(holding)


def bell_draw(key, shape, spread, most, pieces=(), kind=jnp.bfloat16):
    result = jax.random.normal(key, shape, jnp.float32) * spread
    if len(pieces) > 0:
        result = block_scale(key, shape, pieces, -0.22, 0.18) * result
    return jnp.clip(result, min=-most, max=most).astype(kind)


def setup_inputs(seed: int = 0) -> dict:
    key_of = jax.random.split(jax.random.key(seed), 13)
    queries = draw_queries(jax.random.fold_in(key_of[12], 71), 0)
    key_rows = draw_key_rows(jax.random.fold_in(key_of[12], 71), 0)
    value_rows = bell_draw(key_of[2], (TOK_A, KV_HEADS * HD), 4.0, 24.0, ((0, 4), (1, 8)))
    sink_logits = jnp.clip(2.0 + 4.0 * jax.random.uniform(key_of[3], (HEADS,), jnp.float32) ** block_scale(key_of[3], (HEADS,), ((0, 8),), -0.2, 0.2), 2.0, 6.0)
    out_weight = bell_draw(key_of[4], (HEADS * HD, D), (HEADS * HD) ** -0.5, 0.125, ((0, 8),))
    expert_input = bell_draw(key_of[5], (TOK_B, D), 1.0, 6.0, ((0, 32),))
    norm_gain = jnp.clip(1.0 + 0.18 * jax.random.normal(key_of[6], (D,), jnp.float32), 0.1, 1.9)
    group_ids_keys = jax.random.split(jax.random.fold_in(key_of[7], 1), TOK_B // TB)
    group_ids_turns = jax.random.permutation(jax.random.fold_in(key_of[7], 3), TOK_B // TB)
    group_ids = jax.vmap(lambda own, number: routed_block(jax.random.fold_in(key_of[7], 2), own, number, TB, N_EP, 1, CAP, 2))(group_ids_keys, group_ids_turns).reshape((TOK_B, 1))
    route_weight = jnp.clip(0.2 + 0.8 * jax.random.uniform(key_of[8], (TOK_B, EXP_DEV), jnp.float32) ** block_scale(key_of[8], (TOK_B, EXP_DEV), ((0, 32),), -0.2, 0.2), 0.2, 1.0)
    gate_weight = bell_draw(key_of[9], (EXPERTS, D, DE), D ** -0.5, 0.125, ((0, 4), (2, 8)))
    up_weight = bell_draw(key_of[10], (EXPERTS, D, DE), D ** -0.5, 0.125, ((0, 4), (2, 8)))
    down_weight = bell_draw(key_of[11], (EXPERTS, DE, D), DE ** -0.5, 0.09375, ((0, 4), (1, 8)))
    return {"queries": queries, "key_rows": key_rows, "value_rows": value_rows, "sink_logits": sink_logits, "out_weight": out_weight, "expert_input": expert_input, "norm_gain": norm_gain, "group_ids": group_ids, "route_weight": route_weight, "gate_weight": gate_weight, "up_weight": up_weight, "down_weight": down_weight}


theta_base = 10000.0
norm_eps = 1e-06
neg_large = -1e+30

def rotate(tensor, positions):
    halfway = tensor.shape[-1] // 2
    frequency = theta_base ** (-(jnp.arange(halfway, dtype=jnp.float32) * 2.0) / tensor.shape[-1])
    angles = positions.astype(jnp.float32)[:, None] * frequency[None, :]
    cosine = jnp.cos(angles)[:, None, :]
    sine_part = jnp.sin(angles)[:, None, :]
    front_part = tensor[..., :halfway]
    back_part = tensor[..., halfway:]
    return jnp.concatenate([front_part * cosine - back_part * sine_part, back_part * cosine + front_part * sine_part], axis=-1)

def attention(queries, key_rows, value_rows, sink_logits, out_weight):
    tokens = queries.shape[0]
    per_group = HEADS // KV_HEADS
    positions = jnp.arange(tokens, dtype=jnp.int32)
    rot_query = rotate(queries.astype(jnp.float32).reshape(tokens, HEADS, HD), positions).astype(jnp.bfloat16)
    rot_key = rotate(key_rows.astype(jnp.float32).reshape(tokens, KV_HEADS, HD), positions).astype(jnp.bfloat16)
    value_heads = value_rows.reshape(tokens, KV_HEADS, HD)
    key_padded = jnp.concatenate([jnp.zeros((WINDOW, KV_HEADS, HD), jnp.bfloat16), rot_key], axis=0)
    value_padded = jnp.concatenate([jnp.zeros((WINDOW, KV_HEADS, HD), jnp.bfloat16), value_heads], axis=0)
    score_scale = 1.0 / math.sqrt(HD)
    row_ids = jnp.arange(WINDOW, dtype=jnp.int32)[:, None]
    col_ids = jnp.arange(2 * WINDOW, dtype=jnp.int32)[None, :]
    lagged = row_ids + WINDOW - col_ids
    sink_col = sink_logits.astype(jnp.float32).reshape(KV_HEADS, per_group, 1, 1)

    def one_block(block_id):
        begin = (block_id * WINDOW).astype(jnp.int32)
        query_blk = lax.dynamic_slice_in_dim(rot_query, begin, WINDOW, 0).reshape(WINDOW, KV_HEADS, per_group, HD)
        key_blk = lax.dynamic_slice_in_dim(key_padded, begin, 2 * WINDOW, 0)
        value_blk = lax.dynamic_slice_in_dim(value_padded, begin, 2 * WINDOW, 0)
        scores = jnp.einsum('qkgd,skd->kgqs', query_blk.astype(jnp.float32), key_blk.astype(jnp.float32)) * score_scale
        key_pos = begin - WINDOW + col_ids
        allowed = (lagged >= 0) & (lagged < WINDOW) & (key_pos >= 0)
        scores = jnp.where(allowed[None, None], scores, neg_large)
        top_val = jnp.maximum(lax.optimization_barrier(jnp.max(scores, axis=-1, keepdims=True)), sink_col)
        expo = jnp.exp(scores - top_val)
        denom = lax.optimization_barrier(jnp.sum(expo, axis=-1, keepdims=True)) + jnp.exp(sink_col - top_val)
        probs = (expo / denom).astype(jnp.bfloat16)
        mixed = jnp.einsum('kgqs,skd->qkgd', probs.astype(jnp.float32), value_blk.astype(jnp.float32))
        return mixed.reshape(WINDOW, HEADS * HD).astype(jnp.bfloat16)
    attended = lax.map(one_block, jnp.arange(tokens // WINDOW, dtype=jnp.int32)).reshape(tokens, HEADS * HD)
    group_cols = HEADS * HD // N_TP

    def add_group(total, group_id):
        cols = lax.dynamic_slice_in_dim(attended, group_id * group_cols, group_cols, 1)
        rows_w = lax.dynamic_slice_in_dim(out_weight, group_id * group_cols, group_cols, 0)
        partial_sum = jnp.dot(cols, rows_w, preferred_element_type=jnp.float32).astype(jnp.bfloat16)
        partial_sum = lax.optimization_barrier(partial_sum)
        return (total + partial_sum.astype(jnp.float32), None)
    total, unused = lax.scan(add_group, jnp.zeros((tokens, D), jnp.float32), jnp.arange(N_TP, dtype=jnp.int32))
    return total.astype(jnp.bfloat16)

def experts(expert_input, norm_gain, group_ids, route_weight, gate_weight, up_weight, down_weight):
    tokens = expert_input.shape[0]
    as_float = expert_input.astype(jnp.float32)
    normed = (as_float * lax.rsqrt(lax.optimization_barrier(jnp.mean(as_float * as_float, axis=-1, keepdims=True)) + norm_eps) * norm_gain).astype(jnp.bfloat16)
    shares = lax.optimization_barrier(route_weight.astype(jnp.bfloat16)).astype(jnp.float32)
    chosen = group_ids[:, 0].astype(jnp.int32)
    nblocks = tokens // TB
    onehot = (chosen.reshape(nblocks, TB)[:, :, None] == jnp.arange(N_EP, dtype=jnp.int32)[None, None, :]).astype(jnp.int32)
    ranks = lax.optimization_barrier(jnp.sum((jnp.cumsum(onehot, axis=1) - onehot) * onehot, axis=-1)).reshape(tokens)
    block_of = jnp.arange(tokens, dtype=jnp.int32) // TB
    dest = ((chosen * nblocks + block_of) * CAP + ranks).astype(jnp.int32)
    slots = N_EP * nblocks * CAP
    slot_rows = jnp.zeros((slots, D), jnp.bfloat16).at[dest].set(normed)
    slot_shares = jnp.zeros((slots, EXP_DEV), jnp.float32).at[dest].set(shares)
    per_group = nblocks * CAP
    unit_group = DE // N_TP

    def one_group(args):
        rows_in, shares_in, group_id = args
        first = (group_id * EXP_DEV).astype(jnp.int32)
        gate_w = lax.dynamic_slice_in_dim(gate_weight, first, EXP_DEV, 0).astype(jnp.float32)
        up_w = lax.dynamic_slice_in_dim(up_weight, first, EXP_DEV, 0).astype(jnp.float32)
        down_w = lax.dynamic_slice_in_dim(down_weight, first, EXP_DEV, 0)
        rows_f = rows_in.astype(jnp.float32)
        gate_val = jnp.einsum('rd,edf->ref', rows_f, gate_w)
        up_val = jnp.einsum('rd,edf->ref', rows_f, up_w)
        hidden = (jax.nn.silu(gate_val) * up_val * shares_in[:, :, None]).astype(jnp.bfloat16)

        def add_units(total, unit_id):
            hid_part = lax.dynamic_slice_in_dim(hidden, unit_id * unit_group, unit_group, 2).astype(jnp.float32)
            down_part = lax.dynamic_slice_in_dim(down_w, unit_id * unit_group, unit_group, 1).astype(jnp.float32)
            partial_sum = jnp.einsum('ref,efd->rd', hid_part, down_part).astype(jnp.bfloat16)
            partial_sum = lax.optimization_barrier(partial_sum)
            return (total + partial_sum.astype(jnp.float32), None)
        total, unused = lax.scan(add_units, jnp.zeros((per_group, D), jnp.float32), jnp.arange(N_TP, dtype=jnp.int32))
        return total.astype(jnp.bfloat16)
    results = lax.map(one_group, (slot_rows.reshape(N_EP, per_group, D), slot_shares.reshape(N_EP, per_group, EXP_DEV), jnp.arange(N_EP, dtype=jnp.int32)))
    return results.reshape(slots, D)[dest]

def reference(queries, key_rows, value_rows, sink_logits, out_weight, expert_input, norm_gain, group_ids, route_weight, gate_weight, up_weight, down_weight):
    attn_output = attention(queries, key_rows, value_rows, sink_logits, out_weight)
    expert_output = experts(expert_input, norm_gain, group_ids, route_weight, gate_weight, up_weight, down_weight)
    return (attn_output, expert_output)
```

```python
import functools
import math

import jax
import jax.numpy as jnp
import numpy as np
from jax import lax
from jax.experimental import pallas as pl
from jax.experimental.pallas import tpu as pltpu
from jax.sharding import PartitionSpec as P


HD = 64
WINDOW = 128
EXP_DEV = 2
CORES = 2


theta_base = 10000.0
norm_eps = 1e-06
neg_large = -1e30
BF = jnp.bfloat16
F32 = jnp.float32


def gather_pairs(n, s, parity):
    pairs = []
    for link in range(parity, n - 1, 2):
        if link >= s - 1:
            pairs.append((link, link + 1))
        if link <= n - 1 - s:
            pairs.append((link + 1, link))
    return pairs


def scatter_pairs(n, s, parity):
    pairs = [(b, a) for a, b in gather_pairs(n, n - s, parity)]
    return [p for p in pairs if p not in first_hop(n)]


def first_hop(n):
    return [(0, 1), (n - 1, n - 2)]


def along(value, pairs):
    full = [(CORES * a + c, CORES * b + c) for a, b in pairs for c in range(CORES)]
    return lax.ppermute(value, "tp", full)


def core_swap(value):
    n = lax.axis_size("tp")
    return lax.ppermute(value, "tp", [(t, t ^ 1) for t in range(n)])


def slot_chunk(n, z, k):
    if k == 0:
        return z
    even = z % 2 == 0
    ec = jnp.where(even, n - 1 - z, z)
    o = n - k
    return jnp.where(
        k <= ec, jnp.where(even, z + k, z - k), jnp.where(even, z - o, z + o)
    )


def add_all(values):
    values = [v[0][v[1]] if isinstance(v, tuple) else v for v in values]
    if len(values) == 1:
        return values[0]
    return sum(v.astype(F32) for v in values).astype(BF)


class Sequence:
    def __init__(self):
        self.token = None

    def after(self, *values):
        arrays = [v[0] if isinstance(v, tuple) else v for v in values]
        arrays = lax.optimization_barrier((*arrays, self.token))[:-1]
        return [
            (a, v[1]) if isinstance(v, tuple) else a for a, v in zip(arrays, values)
        ]

    def did(self, value):
        self.token = value
        return value


class LineScatter:
    def __init__(self, n, seq):
        self.n = n
        self.seq = seq
        self.first = {}
        self.got = {}

    def send(self, values, pairs):
        out = add_all(self.seq.after(*values))
        if len(values) > 1:
            self.seq.did(out)
        return along(out, pairs)

    def start(self, s, slot):
        self.first[s] = self.send(slot, first_hop(self.n))

    def arrivals(self, s, parity):
        values = [self.got.get((s, parity))]
        if parity == 0:
            values.append(self.first.get(s))
        return [v for v in values if v is not None]

    def step(self, s, slots):
        for parity in (1, 0):
            pairs = scatter_pairs(self.n, s, parity)
            if pairs:
                slot = slots[self.n - s] if parity == 0 else slots[s]
                values = slot + self.arrivals(s - 1, 1 - parity)
                self.got[s, parity] = self.send(values, pairs)

    def finish(self, slot):
        last = self.n - 1
        return slot + self.arrivals(last, 0) + self.arrivals(last, 1)


def round_up(value, to):
    return -(-value // to) * to


def iota(shape, dim):
    return lax.broadcasted_iota(jnp.int32, shape, dim)


def routing(ids_ref, me_ref, block):
    ids = ids_ref[...].astype(F32)
    tokens = ids.shape[1]
    sq_row, sq_col = iota((tokens, tokens), 0), iota((tokens, tokens), 1)
    ids_col = jnp.sum(jnp.where(sq_row == sq_col, ids, 0.0), axis=1, keepdims=True)
    earlier = (ids_col == ids) & (sq_row < sq_col)
    rank = jnp.sum(earlier.astype(F32), axis=0, keepdims=True)
    group = (ids_ref[...] ^ me_ref[0]).astype(F32)
    slot = group * block + rank
    slot_col = jnp.sum(jnp.where(sq_row == sq_col, slot, 0.0), axis=1, keepdims=True)
    return group, rank, slot, slot_col


def dispatch_kernel(
    capacity, block, me_ref, x_ref, gain_ref, ids_ref, share_ref, k_ref, v_ref, *out_refs
):
    *out_refs, tail_ref = out_refs
    tail_ref[:WINDOW] = k_ref[...]
    tail_ref[WINDOW:] = v_ref[...]
    rows = len(out_refs) * block
    tokens = x_ref.shape[0]
    lanes = 128
    x = x_ref[...].astype(F32)
    scale = lax.rsqrt(jnp.mean(x * x, axis=-1, keepdims=True) + norm_eps)
    normed = (x * scale * gain_ref[...]).astype(BF)
    group, rank, slot, _ = routing(ids_ref, me_ref, block)
    row_id = iota((rows, tokens), 0)
    picker = (row_id.astype(F32) == slot).astype(BF)
    out = jnp.dot(picker, normed, preferred_element_type=F32)
    place = row_id % block - capacity
    same = (row_id // block).astype(F32) == group
    weight = jnp.zeros((rows, tokens), F32)
    for k in range(EXP_DEV):
        share = share_ref[k : k + 1, :].astype(BF).astype(F32)
        weight = jnp.where(same & (place == k), share, weight)
    sq_row, sq_col = iota((tokens, tokens), 0), iota((tokens, tokens), 1)
    rank_col = jnp.sum(jnp.where(sq_row == sq_col, rank, 0.0), axis=1, keepdims=True)
    by_rank = (rank_col == iota((tokens, lanes), 1).astype(F32)).astype(BF)
    tail = jnp.dot(weight.astype(BF), by_rank, preferred_element_type=F32)
    for g, out_ref in enumerate(out_refs):
        part = slice(g * block, (g + 1) * block)
        out_ref[:, :lanes] = (out[part, :lanes] + tail[part]).astype(BF)
        out_ref[:, lanes:] = out[part, lanes:].astype(BF)


def in_vmem(count):
    return [pl.BlockSpec(memory_space=pltpu.VMEM)] * count


def dispatch(me, x, gain, ids, share, keys, values, n_groups, capacity, block):
    rows, narrow = keys.shape
    gain = gain.reshape(1, -1)
    last = pl.BlockSpec((WINDOW, narrow), lambda i: (rows // WINDOW - 1, 0))

    def whole(shape):
        return pl.BlockSpec(shape, lambda i: (0, 0))

    outs = [(block, x.shape[1])] * n_groups + [(2 * WINDOW, narrow)]
    return pl.pallas_call(
        functools.partial(dispatch_kernel, capacity, block),
        grid=(1,),
        in_specs=[pl.BlockSpec(memory_space=pltpu.SMEM)]
        + [whole(v.shape) for v in (x, gain, ids, share)]
        + [last, last],
        out_specs=[whole(o) for o in outs],
        out_shape=[jax.ShapeDtypeStruct(o, BF) for o in outs],
        compiler_params=pltpu.CompilerParams(vmem_limit_bytes=60 << 20),
        name="dispatch",
    )(me, x, gain, ids, share, keys, values)


def pack_kernel(*refs):
    *parts, out_ref = refs
    block = parts[0].shape[0]
    for i, part in enumerate(parts):
        out_ref[i * block : (i + 1) * block] = part[...]


def pack(parts):
    block, width = parts[0].shape
    return pl.pallas_call(
        pack_kernel,
        in_specs=in_vmem(len(parts)),
        out_specs=in_vmem(1)[0],
        out_shape=jax.ShapeDtypeStruct((len(parts) * block, width), BF),
        compiler_params=pltpu.CompilerParams(vmem_limit_bytes=16 << 20),
        name="pack",
    )(*parts)


def combine_kernel(block, me_ref, ids_ref, *refs):
    *parts, out_ref = refs
    tokens = out_ref.shape[0]
    slot_col = routing(ids_ref, me_ref, block)[3]
    rows = jnp.concatenate([p[...] for p in parts], axis=0)
    picker = (slot_col == iota((tokens, rows.shape[0]), 1).astype(F32)).astype(BF)
    out_ref[...] = jnp.dot(picker, rows, preferred_element_type=F32).astype(BF)


def combine(me, ids, parts):
    block, width = parts[0].shape
    return pl.pallas_call(
        functools.partial(combine_kernel, block),
        in_specs=[pl.BlockSpec(memory_space=pltpu.SMEM)] + in_vmem(1 + len(parts)),
        out_shape=jax.ShapeDtypeStruct((ids.shape[1], width), BF),
        compiler_params=pltpu.CompilerParams(vmem_limit_bytes=16 << 20),
        name="combine",
    )(me, ids, *parts)


def expert_kernel(capacity, block, count, *refs):
    parts, refs = refs[:count], refs[count:]
    gate_ref, up_ref, down_ref = refs[:3]
    outs = refs[3 : 3 + count]
    x_s, h_s = refs[3 + count :]
    half = parts[0].shape[0]
    units = gate_ref.shape[2]
    for i, part in enumerate(parts):
        x_s[i * half : (i + 1) * half] = part[...]
    row, col = iota((half, half), 0), iota((half, half), 1)
    mine = iota((half, 128), 0) % block == iota((half, 128), 1)
    shares = []
    for k in range(EXP_DEV):
        take = (col == row - row % block + capacity + k).astype(BF)
        columns = []
        for part in parts:
            spread = jnp.dot(take, part[:, :128], preferred_element_type=F32)
            columns.append(jnp.sum(jnp.where(mine, spread, 0.0), axis=1, keepdims=True))
        shares.append(jnp.concatenate(columns, axis=0))
    cut = math.gcd(units, 256)
    for k in range(EXP_DEV):
        for c in range(0, units, cut):
            x = x_s[...]
            gate = jnp.dot(x, gate_ref[k, :, c : c + cut], preferred_element_type=F32)
            up = jnp.dot(x, up_ref[k, :, c : c + cut], preferred_element_type=F32)
            hidden = gate / (1.0 + jnp.exp(-gate)) * up * shares[k]
            h_s[:, k * units + c : k * units + c + cut] = hidden.astype(BF)
    width = x_s.shape[1]
    piece = math.gcd(width, 512)
    for c in range(0, width, piece):
        total = jnp.dot(h_s[...], down_ref[:, c : c + piece], preferred_element_type=F32)
        for i, out in enumerate(outs):
            out[:, c : c + piece] = total[i * half : (i + 1) * half].astype(BF)


def expert_rows(parts, gate, up, down, capacity, block):
    count = len(parts)
    half, width = parts[0].shape
    units = gate.shape[2]
    return pl.pallas_call(
        functools.partial(expert_kernel, capacity, block, count),
        in_specs=in_vmem(count + 3),
        out_specs=in_vmem(count),
        out_shape=[jax.ShapeDtypeStruct((half, width), BF)] * count,
        scratch_shapes=[
            pltpu.VMEM((count * half, width), BF),
            pltpu.VMEM((count * half, EXP_DEV * units), BF),
        ],
        cost_estimate=pl.CostEstimate(
            flops=2 * count * half * width * units * EXP_DEV * 3,
            bytes_accessed=4 * count * half * width,
            transcendentals=count * half * units * EXP_DEV,
        ),
        compiler_params=pltpu.CompilerParams(vmem_limit_bytes=24 << 20),
        name="experts",
    )(*parts, gate, up, down)


def attention_kernel(
    kv_here,
    per_group,
    many,
    order_ref,
    base_ref,
    sink_ref,
    q_ref,
    k_ref,
    v_ref,
    tail_ref,
    step_ref,
    start_ref,
    turn_ref,
    w_ref,
    *rest,
):
    span = WINDOW
    turn = turn_ref[...]
    plus_ref = rest[0] if len(rest) > 1 else None
    outs = rest[1:]
    step = pl.program_id(0)
    shape = (per_group * span, 2 * span)
    row = lax.broadcasted_iota(jnp.int32, shape, 0)
    col = lax.broadcasted_iota(jnp.int32, shape, 1)
    lag = row % span + span - col
    inside = (lag >= 0) & (lag < span)
    column = lax.broadcasted_iota(jnp.int32, (per_group * span, 1), 0) // span
    sinks = []
    for c in range(kv_here):
        sink = jnp.full((per_group * span, 1), sink_ref[c * per_group], F32)
        for g in range(1, per_group):
            sink = jnp.where(column == g, sink_ref[c * per_group + g], sink)
        sinks.append(sink)

    def rotated(x, at, scale):
        width = x.shape[1]
        cos_i, sin_i = step_ref[0, :, :width], step_ref[1, :, :width]
        base = start_ref[at]
        cos_0, sin_0 = base[0:1, :width], base[1:2, :width]
        cosine = cos_0 * cos_i - sin_0 * sin_i
        sine = sin_0 * cos_i + cos_0 * sin_i
        swapped = jnp.dot(x, turn[:width, :width], preferred_element_type=F32)
        return ((x.astype(F32) * cosine + swapped * sine) * scale).astype(BF)

    for b in range(many):
        index = order_ref[step * many + b]
        first = index == 0
        place = base_ref[0] + index
        here = pl.ds(pl.multiple_of(index * span, span), span)
        back = pl.ds(pl.multiple_of(jnp.maximum(index - 1, 0) * span, span), span)
        q = rotated(q_ref[here, :], place, 1.0 / math.sqrt(HD))
        before_k = jnp.where(first, tail_ref[:span], k_ref[back, :])
        before_v = jnp.where(first, tail_ref[span:], v_ref[back, :])
        keys = jnp.concatenate(
            [
                rotated(before_k, jnp.maximum(place - 1, 0), 1.0),
                rotated(k_ref[here, :], place, 1.0),
            ],
            axis=0,
        )
        values = jnp.concatenate([before_v, v_ref[here, :]], axis=0)
        allowed = inside & (col >= jnp.where(place == 0, span, 0))
        attended = []
        for c in range(kv_here):
            heads = [c * per_group + g for g in range(per_group)]
            rows = jnp.concatenate([q[:, h * HD : (h + 1) * HD] for h in heads], axis=0)
            key = keys[:, c * HD : (c + 1) * HD]
            scores = lax.dot_general(
                rows, key, (((1,), (1,)), ((), ())), preferred_element_type=F32
            )
            scores = jnp.where(allowed, scores, neg_large)
            top = jnp.maximum(jnp.max(scores, axis=1, keepdims=True), sinks[c])
            expo = jnp.exp(scores - top)
            denom = jnp.sum(expo, axis=1, keepdims=True) + jnp.exp(sinks[c] - top)
            mixed = jnp.dot(
                expo.astype(BF), values[:, c * HD : (c + 1) * HD], preferred_element_type=F32
            )
            mixed = (mixed / denom).astype(BF)
            attended += [mixed[g * span : (g + 1) * span] for g in range(per_group)]
        attended = jnp.concatenate(attended, axis=1)
        total = jnp.dot(attended, w_ref[...], preferred_element_type=F32)
        if plus_ref is None:
            rest[0][b] = total.astype(BF)
            continue
        total = (total + plus_ref[b].astype(F32)).astype(BF)
        for i in range(b, len(outs), many):

            @pl.when(step == i // many)
            def _(i=i):
                outs[i][...] = total


def rotary_tables(width, blocks):
    half = HD // 2
    frequency = theta_base ** (-(np.arange(half, dtype=np.float64) * 2.0) / HD)
    lanes = np.tile(frequency, width // half)[None, :]
    inside = np.arange(WINDOW)[:, None] * lanes
    starts = (np.arange(blocks) * WINDOW)[:, None] * lanes
    steps = np.stack([np.cos(inside), np.sin(inside)]).astype(np.float32)
    bases = np.stack([np.cos(starts), np.sin(starts)], axis=1).astype(np.float32)
    lane = np.arange(width)
    turn = np.zeros((width, width), np.float32)
    low = lane % HD < half
    turn[np.where(low, lane + half, lane - half), lane] = np.where(low, -1.0, 1.0)
    return steps, bases, turn


def attention_partials(
    order, base, queries, keys, values, tails, sinks, weight, blocks, plus=None
):
    width = queries.shape[1]
    narrow = keys.shape[1]
    kv_here = narrow // HD
    per_group = width // narrow
    count = order.shape[0]
    steps, bases, turn = rotary_tables(width, blocks)
    many = math.gcd(count, 2)
    operands = (
        queries,
        keys,
        values,
        tails,
        jnp.asarray(steps),
        jnp.asarray(bases),
        jnp.asarray(turn, BF),
        weight,
    )

    def fixed(x):
        return pl.BlockSpec(x.shape, lambda i, o, b, s: (0,) * len(x.shape))

    out_width = weight.shape[1]
    stack = pl.BlockSpec((many, WINDOW, out_width), lambda i, o, b, s: (i, 0, 0))
    in_specs = [fixed(x) for x in operands]
    if plus is None:
        out_specs, out_shape = stack, jax.ShapeDtypeStruct((count, WINDOW, out_width), BF)
    else:
        operands += (plus,)
        in_specs += [stack]
        out_shape = [jax.ShapeDtypeStruct((WINDOW, out_width), BF)] * count
        out_specs = [fixed(o) for o in out_shape]
    return pl.pallas_call(
        functools.partial(attention_kernel, kv_here, per_group, many),
        grid_spec=pltpu.PrefetchScalarGridSpec(
            num_scalar_prefetch=3,
            grid=(count // many,),
            in_specs=in_specs,
            out_specs=out_specs,
        ),
        out_shape=out_shape,
        cost_estimate=pl.CostEstimate(
            flops=2 * count * WINDOW * width * (weight.shape[1] + 4 * WINDOW),
            bytes_accessed=2 * weight.size + 2 * count * WINDOW * (weight.shape[1] + 2 * width),
            transcendentals=count * WINDOW * 2 * WINDOW * kv_here * per_group,
        ),
        compiler_params=pltpu.CompilerParams(vmem_limit_bytes=(60 if plus is None else 28) << 20),
        name="attention",
    )(order, base, sinks, *operands)


def body(
    queries,
    key_rows,
    value_rows,
    sink_logits,
    out_weight,
    expert_input,
    norm_gain,
    group_ids,
    route_weight,
    gate_weight,
    up_weight,
    down_weight,
):
    n_groups = lax.axis_size("ep")
    n_tp = lax.axis_size("tp")
    n = n_tp // CORES
    token_count, width = expert_input.shape
    capacity = max(2, token_count * 5 // (4 * n_groups))
    block = round_up(capacity + EXP_DEV, 8)
    e = lax.axis_index("ep")
    t = lax.axis_index("tp")
    z, core = t // CORES, t % CORES
    me = e.reshape(1)
    ids = group_ids.reshape(1, token_count)
    seq = Sequence()

    def around(part, k):
        return lax.ppermute(part, "ep", [(i, i ^ k) for i in range(n_groups)])

    *send, tails = dispatch(
        me,
        expert_input,
        norm_gain,
        ids,
        route_weight.T,
        key_rows,
        value_rows,
        n_groups,
        capacity,
        block,
    )
    seq.did(send[0])
    got = [send[0]] + [around(send[k], k) for k in range(1, n_groups)]

    before = lax.ppermute(tails, "ep", [(i, i + 1) for i in range(n_groups - 1)])
    chunk = jnp.stack([slot_chunk(n, z, k) for k in range(n)]) * CORES

    def attend(order, plus=None):
        (q,) = seq.after(queries)
        return attention_partials(
            order,
            (e * n_tp).reshape(1),
            q,
            key_rows,
            value_rows,
            before,
            sink_logits,
            out_weight,
            n_groups * n_tp,
            plus,
        )

    arrived = {}

    def gather(s):
        for parity in (1, 0):
            pairs = gather_pairs(n, s, parity)
            if pairs:
                value = own
                if s > 1:
                    (value,) = seq.after(arrived[s - 1, 1 - parity])
                arrived[s, parity] = along(value, pairs)

    slots = {}

    def prepare(s):
        for k in range(1, n):
            late = n - k if gather_pairs(n, n - k, 1) else 0
            if max(k, late) == s:
                addends = [arrived[k, 0], arrived.get((n - k, 1))]
                slot = add_all([a for a in addends if a is not None])
                slots[k] = [slot, core_swap(slot)]

    back = {}

    def experts(ks):
        for k in ks:
            parts = seq.after(*slots[k])
            done = expert_rows(parts, *weights, capacity, block)
            seq.did(done[0])
            back[k] = [done[0], core_swap(done[1])]

    own = seq.did(pack(seq.after(*got)))
    gather(1)
    slots[0] = [own, core_swap(own)]
    other = seq.did(attend(chunk + 1 - core))
    swapped = core_swap(other)
    weights = seq.after(gate_weight, up_weight, down_weight.reshape(-1, width))
    attn_scatter = LineScatter(n, seq)
    for s in range(1, n):
        todo = [k for k in slots if k not in back]
        if s == n - 1:
            experts(todo)
        else:
            gather(s + 1)
        prepare(s)
        if s == 1:
            (swapped,) = seq.after(swapped)
            mine = attend(chunk + core, swapped)
            seq.did(mine[0])
            attn = [[v] for v in mine]
            for a in range(1, n):
                attn_scatter.start(a, attn[n - a])
        elif s < n - 1:
            experts(todo[:1])
            attn_scatter.step(s, attn)
            experts(todo[1:])
    experts([k for k in slots if k not in back])
    attn_scatter.step(n - 1, attn)

    scatter = LineScatter(n, seq)
    for s in range(1, n):
        scatter.start(s, back[n - s])
    for s in range(2, n):
        scatter.step(s, back)
    attn_output = seq.did(add_all(seq.after(*attn_scatter.finish(attn[0]))))
    addends = seq.after(*scatter.finish(back[0]))
    home = []
    for k in range(n_groups):
        part = add_all([v[k * block : (k + 1) * block] for v in addends])
        home.append(around(part, k) if k else part)
    expert_output = combine(me, ids, home)
    return (attn_output, expert_output)


def solution(mesh):
    placed = (
        P("ep", "tp"),
        P("ep", "tp"),
        P("ep", "tp"),
        P("tp"),
        P("tp", None),
        P(("ep", "tp"), None),
        P(),
        P(("ep", "tp"), None),
        P(("ep", "tp"), None),
        P("ep", None, "tp"),
        P("ep", None, "tp"),
        P("ep", "tp", None),
    )
    return jax.shard_map(
        body,
        mesh=mesh,
        in_specs=placed,
        out_specs=(P(("ep", "tp"), None), P(("ep", "tp"), None)),
        check_vma=False,
    )
```

```python
import functools
import math

import jax
import jax.numpy as jnp
import numpy as np
from jax import lax
from jax.experimental import pallas as pl
from jax.experimental.pallas import tpu as pltpu
from jax.sharding import PartitionSpec as P


HD = 64
WINDOW = 128
EXP_DEV = 2
CORES = 2


theta_base = 10000.0
norm_eps = 1e-06
neg_large = -1e30
BF = jnp.bfloat16
F32 = jnp.float32


def gather_pairs(n, s, parity):
    pairs = []
    for link in range(parity, n - 1, 2):
        if link >= s - 1:
            pairs.append((link, link + 1))
        if link <= n - 1 - s:
            pairs.append((link + 1, link))
    return pairs


def scatter_pairs(n, s, parity):
    pairs = [(b, a) for a, b in gather_pairs(n, n - s, parity)]
    return [p for p in pairs if p not in first_hop(n)]


def first_hop(n):
    return [(0, 1), (n - 1, n - 2)]


def along(value, pairs):
    full = [(CORES * a + c, CORES * b + c) for a, b in pairs for c in range(CORES)]
    return lax.ppermute(value, "tp", full)


def core_swap(value):
    n = lax.axis_size("tp")
    return lax.ppermute(value, "tp", [(t, t ^ 1) for t in range(n)])


def slot_chunk(n, z, k):
    if k == 0:
        return z
    even = z % 2 == 0
    ec = jnp.where(even, n - 1 - z, z)
    o = n - k
    return jnp.where(
        k <= ec, jnp.where(even, z + k, z - k), jnp.where(even, z - o, z + o)
    )


def add_all(values):
    values = [v[0][v[1]] if isinstance(v, tuple) else v for v in values]
    if len(values) == 1:
        return values[0]
    return sum(v.astype(F32) for v in values).astype(BF)


class Sequence:
    def __init__(self):
        self.token = None

    def after(self, *values):
        arrays = [v[0] if isinstance(v, tuple) else v for v in values]
        arrays = lax.optimization_barrier((*arrays, self.token))[:-1]
        return [
            (a, v[1]) if isinstance(v, tuple) else a for a, v in zip(arrays, values)
        ]

    def did(self, value):
        self.token = value
        return value


class LineScatter:
    def __init__(self, n, seq):
        self.n = n
        self.seq = seq
        self.first = {}
        self.got = {}

    def send(self, values, pairs):
        out = add_all(self.seq.after(*values))
        if len(values) > 1:
            self.seq.did(out)
        return along(out, pairs)

    def start(self, s, slot):
        self.first[s] = self.send(slot, first_hop(self.n))

    def arrivals(self, s, parity):
        values = [self.got.get((s, parity))]
        if parity == 0:
            values.append(self.first.get(s))
        return [v for v in values if v is not None]

    def step(self, s, slots):
        for parity in (0, 1):
            pairs = scatter_pairs(self.n, s, parity)
            if pairs:
                slot = slots[self.n - s] if parity == 0 else slots[s]
                values = slot + self.arrivals(s - 1, 1 - parity)
                self.got[s, parity] = self.send(values, pairs)

    def finish(self, slot):
        last = self.n - 1
        return slot + self.arrivals(last, 0) + self.arrivals(last, 1)


def round_up(value, to):
    return -(-value // to) * to


def iota(shape, dim):
    return lax.broadcasted_iota(jnp.int32, shape, dim)


def routing(ids_ref, me_ref, block):
    ids = ids_ref[...].astype(F32)
    tokens = ids.shape[1]
    sq_row, sq_col = iota((tokens, tokens), 0), iota((tokens, tokens), 1)
    ids_col = jnp.sum(jnp.where(sq_row == sq_col, ids, 0.0), axis=1, keepdims=True)
    earlier = (ids_col == ids) & (sq_row < sq_col)
    rank = jnp.sum(earlier.astype(F32), axis=0, keepdims=True)
    group = (ids_ref[...] ^ me_ref[0]).astype(F32)
    slot = group * block + rank
    slot_col = jnp.sum(jnp.where(sq_row == sq_col, slot, 0.0), axis=1, keepdims=True)
    return group, rank, slot, slot_col


def tails_kernel(k_ref, v_ref, tail_ref):
    tail_ref[:WINDOW] = k_ref[...]
    tail_ref[WINDOW:] = v_ref[...]


def last_rows(keys, values):
    rows, narrow = keys.shape
    last = pl.BlockSpec((WINDOW, narrow), lambda i: (rows // WINDOW - 1, 0))
    return pl.pallas_call(
        tails_kernel,
        grid=(1,),
        in_specs=[last, last],
        out_specs=pl.BlockSpec((2 * WINDOW, narrow), lambda i: (0, 0)),
        out_shape=jax.ShapeDtypeStruct((2 * WINDOW, narrow), BF),
        compiler_params=pltpu.CompilerParams(vmem_limit_bytes=60 << 20),
        name="last_rows",
    )(keys, values)


def dispatch_kernel(capacity, block, me_ref, x_ref, gain_ref, ids_ref, share_ref, *out_refs):
    rows = len(out_refs) * block
    tokens = x_ref.shape[0]
    lanes = 128
    x = x_ref[...].astype(F32)
    scale = lax.rsqrt(jnp.mean(x * x, axis=-1, keepdims=True) + norm_eps)
    normed = (x * scale * gain_ref[...]).astype(BF)
    group, rank, slot, _ = routing(ids_ref, me_ref, block)
    row_id = iota((rows, tokens), 0)
    picker = (row_id.astype(F32) == slot).astype(BF)
    out = jnp.dot(picker, normed, preferred_element_type=F32)
    place = row_id % block - capacity
    same = (row_id // block).astype(F32) == group
    weight = jnp.zeros((rows, tokens), F32)
    for k in range(EXP_DEV):
        share = share_ref[k : k + 1, :].astype(BF).astype(F32)
        weight = jnp.where(same & (place == k), share, weight)
    sq_row, sq_col = iota((tokens, tokens), 0), iota((tokens, tokens), 1)
    rank_col = jnp.sum(jnp.where(sq_row == sq_col, rank, 0.0), axis=1, keepdims=True)
    by_rank = (rank_col == iota((tokens, lanes), 1).astype(F32)).astype(BF)
    tail = jnp.dot(weight.astype(BF), by_rank, preferred_element_type=F32)
    for g, out_ref in enumerate(out_refs):
        part = slice(g * block, (g + 1) * block)
        out_ref[:, :lanes] = (out[part, :lanes] + tail[part]).astype(BF)
        out_ref[:, lanes:] = out[part, lanes:].astype(BF)


def in_vmem(count):
    return [pl.BlockSpec(memory_space=pltpu.VMEM)] * count


def dispatch(me, x, gain, ids, share, n_groups, capacity, block):
    gain = gain.reshape(1, -1)

    def whole(shape):
        return pl.BlockSpec(shape, lambda i: (0, 0))

    outs = [(block, x.shape[1])] * n_groups
    return pl.pallas_call(
        functools.partial(dispatch_kernel, capacity, block),
        grid=(1,),
        in_specs=[pl.BlockSpec(memory_space=pltpu.SMEM)]
        + [whole(v.shape) for v in (x, gain, ids, share)],
        out_specs=[whole(o) for o in outs],
        out_shape=[jax.ShapeDtypeStruct(o, BF) for o in outs],
        compiler_params=pltpu.CompilerParams(vmem_limit_bytes=60 << 20),
        name="dispatch",
    )(me, x, gain, ids, share)


def pack_kernel(*refs):
    *parts, out_ref = refs
    block = parts[0].shape[0]
    for i, part in enumerate(parts):
        out_ref[i * block : (i + 1) * block] = part[...]


def pack(parts):
    block, width = parts[0].shape
    return pl.pallas_call(
        pack_kernel,
        in_specs=in_vmem(len(parts)),
        out_specs=in_vmem(1)[0],
        out_shape=jax.ShapeDtypeStruct((len(parts) * block, width), BF),
        compiler_params=pltpu.CompilerParams(vmem_limit_bytes=16 << 20),
        name="pack",
    )(*parts)


def combine_kernel(block, me_ref, ids_ref, *refs):
    *parts, out_ref = refs
    tokens = out_ref.shape[0]
    slot_col = routing(ids_ref, me_ref, block)[3]
    rows = jnp.concatenate([p[...] for p in parts], axis=0)
    picker = (slot_col == iota((tokens, rows.shape[0]), 1).astype(F32)).astype(BF)
    out_ref[...] = jnp.dot(picker, rows, preferred_element_type=F32).astype(BF)


def combine(me, ids, parts):
    block, width = parts[0].shape
    return pl.pallas_call(
        functools.partial(combine_kernel, block),
        in_specs=[pl.BlockSpec(memory_space=pltpu.SMEM)] + in_vmem(1 + len(parts)),
        out_shape=jax.ShapeDtypeStruct((ids.shape[1], width), BF),
        compiler_params=pltpu.CompilerParams(vmem_limit_bytes=16 << 20),
        name="combine",
    )(me, ids, *parts)


def expert_kernel(capacity, block, count, *refs):
    parts, refs = refs[:count], refs[count:]
    gate_ref, up_ref, down_ref = refs[:3]
    outs = refs[3 : 3 + count]
    x_s, h_s = refs[3 + count :]
    half = parts[0].shape[0]
    units = gate_ref.shape[2]
    for i, part in enumerate(parts):
        x_s[i * half : (i + 1) * half] = part[...]
    row, col = iota((half, half), 0), iota((half, half), 1)
    mine = iota((half, 128), 0) % block == iota((half, 128), 1)
    shares = []
    for k in range(EXP_DEV):
        take = (col == row - row % block + capacity + k).astype(BF)
        columns = []
        for part in parts:
            spread = jnp.dot(take, part[:, :128], preferred_element_type=F32)
            columns.append(jnp.sum(jnp.where(mine, spread, 0.0), axis=1, keepdims=True))
        shares.append(jnp.concatenate(columns, axis=0))
    cut = math.gcd(units, 256)
    for k in range(EXP_DEV):
        for c in range(0, units, cut):
            x = x_s[...]
            gate = jnp.dot(x, gate_ref[k, :, c : c + cut], preferred_element_type=F32)
            up = jnp.dot(x, up_ref[k, :, c : c + cut], preferred_element_type=F32)
            hidden = gate / (1.0 + jnp.exp(-gate)) * up * shares[k]
            h_s[:, k * units + c : k * units + c + cut] = hidden.astype(BF)
    width = x_s.shape[1]
    piece = math.gcd(width, 512)
    for c in range(0, width, piece):
        total = jnp.dot(h_s[...], down_ref[:, c : c + piece], preferred_element_type=F32)
        for i, out in enumerate(outs):
            out[:, c : c + piece] = total[i * half : (i + 1) * half].astype(BF)


def expert_rows(parts, gate, up, down, capacity, block):
    count = len(parts)
    half, width = parts[0].shape
    units = gate.shape[2]
    return pl.pallas_call(
        functools.partial(expert_kernel, capacity, block, count),
        in_specs=in_vmem(count + 3),
        out_specs=in_vmem(count),
        out_shape=[jax.ShapeDtypeStruct((half, width), BF)] * count,
        scratch_shapes=[
            pltpu.VMEM((count * half, width), BF),
            pltpu.VMEM((count * half, EXP_DEV * units), BF),
        ],
        cost_estimate=pl.CostEstimate(
            flops=2 * count * half * width * units * EXP_DEV * 3,
            bytes_accessed=4 * count * half * width,
            transcendentals=count * half * units * EXP_DEV,
        ),
        compiler_params=pltpu.CompilerParams(vmem_limit_bytes=24 << 20),
        name="experts",
    )(*parts, gate, up, down)


def attention_kernel(
    kv_here,
    per_group,
    many,
    order_ref,
    base_ref,
    sink_ref,
    q_ref,
    k_ref,
    v_ref,
    tail_ref,
    step_ref,
    start_ref,
    turn_ref,
    w_ref,
    *rest,
):
    span = WINDOW
    turn = turn_ref[...]
    plus_ref = rest[0] if len(rest) > 1 else None
    outs = rest[1:]
    step = pl.program_id(0)
    shape = (per_group * span, 2 * span)
    row = lax.broadcasted_iota(jnp.int32, shape, 0)
    col = lax.broadcasted_iota(jnp.int32, shape, 1)
    lag = row % span + span - col
    inside = (lag >= 0) & (lag < span)
    column = lax.broadcasted_iota(jnp.int32, (per_group * span, 1), 0) // span
    sinks = []
    for c in range(kv_here):
        sink = jnp.full((per_group * span, 1), sink_ref[c * per_group], F32)
        for g in range(1, per_group):
            sink = jnp.where(column == g, sink_ref[c * per_group + g], sink)
        sinks.append(sink)

    def rotated(x, at, scale):
        width = x.shape[1]
        cos_i, sin_i = step_ref[0, :, :width], step_ref[1, :, :width]
        base = start_ref[at]
        cos_0, sin_0 = base[0:1, :width], base[1:2, :width]
        cosine = cos_0 * cos_i - sin_0 * sin_i
        sine = sin_0 * cos_i + cos_0 * sin_i
        swapped = jnp.dot(x, turn[:width, :width], preferred_element_type=F32)
        return ((x.astype(F32) * cosine + swapped * sine) * scale).astype(BF)

    for b in range(many):
        index = order_ref[step * many + b]
        first = index == 0
        place = base_ref[0] + index
        here = pl.ds(pl.multiple_of(index * span, span), span)
        back = pl.ds(pl.multiple_of(jnp.maximum(index - 1, 0) * span, span), span)
        q = rotated(q_ref[here, :], place, 1.0 / math.sqrt(HD))
        before_k = jnp.where(first, tail_ref[:span], k_ref[back, :])
        before_v = jnp.where(first, tail_ref[span:], v_ref[back, :])
        keys = jnp.concatenate(
            [
                rotated(before_k, jnp.maximum(place - 1, 0), 1.0),
                rotated(k_ref[here, :], place, 1.0),
            ],
            axis=0,
        )
        values = jnp.concatenate([before_v, v_ref[here, :]], axis=0)
        allowed = inside & (col >= jnp.where(place == 0, span, 0))
        attended = []
        for c in range(kv_here):
            heads = [c * per_group + g for g in range(per_group)]
            rows = jnp.concatenate([q[:, h * HD : (h + 1) * HD] for h in heads], axis=0)
            key = keys[:, c * HD : (c + 1) * HD]
            scores = lax.dot_general(
                rows, key, (((1,), (1,)), ((), ())), preferred_element_type=F32
            )
            scores = jnp.where(allowed, scores, neg_large)
            top = jnp.maximum(jnp.max(scores, axis=1, keepdims=True), sinks[c])
            expo = jnp.exp(scores - top)
            denom = jnp.sum(expo, axis=1, keepdims=True) + jnp.exp(sinks[c] - top)
            mixed = jnp.dot(
                expo.astype(BF), values[:, c * HD : (c + 1) * HD], preferred_element_type=F32
            )
            mixed = (mixed / denom).astype(BF)
            attended += [mixed[g * span : (g + 1) * span] for g in range(per_group)]
        attended = jnp.concatenate(attended, axis=1)
        total = jnp.dot(attended, w_ref[...], preferred_element_type=F32)
        if plus_ref is None:
            rest[0][b] = total.astype(BF)
            continue
        total = (total + plus_ref[b].astype(F32)).astype(BF)
        for i in range(b, len(outs), many):

            @pl.when(step == i // many)
            def _(i=i):
                outs[i][...] = total


def rotary_tables(width, blocks):
    half = HD // 2
    frequency = theta_base ** (-(np.arange(half, dtype=np.float64) * 2.0) / HD)
    lanes = np.tile(frequency, width // half)[None, :]
    inside = np.arange(WINDOW)[:, None] * lanes
    starts = (np.arange(blocks) * WINDOW)[:, None] * lanes
    steps = np.stack([np.cos(inside), np.sin(inside)]).astype(np.float32)
    bases = np.stack([np.cos(starts), np.sin(starts)], axis=1).astype(np.float32)
    lane = np.arange(width)
    turn = np.zeros((width, width), np.float32)
    low = lane % HD < half
    turn[np.where(low, lane + half, lane - half), lane] = np.where(low, -1.0, 1.0)
    return steps, bases, turn


def attention_partials(
    order, base, queries, keys, values, tails, sinks, weight, blocks, plus=None
):
    width = queries.shape[1]
    narrow = keys.shape[1]
    kv_here = narrow // HD
    per_group = width // narrow
    count = order.shape[0]
    steps, bases, turn = rotary_tables(width, blocks)
    many = math.gcd(count, 2)
    operands = (
        queries,
        keys,
        values,
        tails,
        jnp.asarray(steps),
        jnp.asarray(bases),
        jnp.asarray(turn, BF),
        weight,
    )

    def fixed(x):
        return pl.BlockSpec(x.shape, lambda i, o, b, s: (0,) * len(x.shape))

    out_width = weight.shape[1]
    stack = pl.BlockSpec((many, WINDOW, out_width), lambda i, o, b, s: (i, 0, 0))
    in_specs = [fixed(x) for x in operands]
    if plus is None:
        out_specs, out_shape = stack, jax.ShapeDtypeStruct((count, WINDOW, out_width), BF)
    else:
        operands += (plus,)
        in_specs += [stack]
        out_shape = [jax.ShapeDtypeStruct((WINDOW, out_width), BF)] * count
        out_specs = [fixed(o) for o in out_shape]
    return pl.pallas_call(
        functools.partial(attention_kernel, kv_here, per_group, many),
        grid_spec=pltpu.PrefetchScalarGridSpec(
            num_scalar_prefetch=3,
            grid=(count // many,),
            in_specs=in_specs,
            out_specs=out_specs,
        ),
        out_shape=out_shape,
        cost_estimate=pl.CostEstimate(
            flops=16 * count * WINDOW * width * (weight.shape[1] + 4 * WINDOW),
            bytes_accessed=2 * weight.size + 2 * count * WINDOW * (weight.shape[1] + 2 * width),
            transcendentals=count * WINDOW * 2 * WINDOW * kv_here * per_group,
        ),
        compiler_params=pltpu.CompilerParams(vmem_limit_bytes=(60 if plus is None else 28) << 20),
        name="attention",
    )(order, base, sinks, *operands)


def body(
    queries,
    key_rows,
    value_rows,
    sink_logits,
    out_weight,
    expert_input,
    norm_gain,
    group_ids,
    route_weight,
    gate_weight,
    up_weight,
    down_weight,
):
    n_groups = lax.axis_size("ep")
    n_tp = lax.axis_size("tp")
    n = n_tp // CORES
    token_count, width = expert_input.shape
    capacity = max(2, token_count * 5 // (4 * n_groups))
    block = round_up(capacity + EXP_DEV, 8)
    e = lax.axis_index("ep")
    t = lax.axis_index("tp")
    z, core = t // CORES, t % CORES
    me = e.reshape(1)
    ids = group_ids.reshape(1, token_count)
    seq = Sequence()

    def around(part, k):
        return lax.ppermute(part, "ep", [(i, i ^ k) for i in range(n_groups)])

    tails = seq.did(last_rows(key_rows, value_rows))
    before = lax.ppermute(tails, "ep", [(i, i + 1) for i in range(n_groups - 1)])
    (x,) = seq.after(expert_input)
    send = dispatch(me, x, norm_gain, ids, route_weight.T, n_groups, capacity, block)
    seq.did(send[0])
    got = [send[0]] + [around(send[k], k) for k in range(1, n_groups)]

    chunk = jnp.stack([slot_chunk(n, z, k) for k in range(n)]) * CORES

    def attend(order, plus=None):
        (q,) = seq.after(queries)
        return attention_partials(
            order,
            (e * n_tp).reshape(1),
            q,
            key_rows,
            value_rows,
            before,
            sink_logits,
            out_weight,
            n_groups * n_tp,
            plus,
        )

    arrived = {}

    def gather(s):
        for parity in (1, 0):
            pairs = gather_pairs(n, s, parity)
            if pairs:
                value = own
                if s > 1:
                    (value,) = seq.after(arrived[s - 1, 1 - parity])
                arrived[s, parity] = along(value, pairs)

    slots = {}

    def prepare(s):
        for k in range(1, n):
            late = n - k if gather_pairs(n, n - k, 1) else 0
            if max(k, late) == s:
                addends = [arrived[k, 0], arrived.get((n - k, 1))]
                slot = add_all([a for a in addends if a is not None])
                slots[k] = [slot, core_swap(slot)]

    back = {}

    def experts(ks):
        for k in ks:
            parts = seq.after(*slots[k])
            done = expert_rows(parts, *weights, capacity, block)
            seq.did(done[0])
            back[k] = [done[0], core_swap(done[1])]

    other = seq.did(attend(chunk + 1 - core))
    swapped = core_swap(other)
    weights = seq.after(gate_weight, up_weight, down_weight.reshape(-1, width))
    own = seq.did(pack(seq.after(*got)))
    gather(1)
    slots[0] = [own, core_swap(own)]
    (swapped,) = seq.after(swapped)
    mine = attend(chunk + core, swapped)
    seq.did(mine[0])
    attn = [[v] for v in mine]
    attn_scatter = LineScatter(n, seq)
    for s in range(1, n):
        if s < n - 1:
            gather(s + 1)
        prepare(s)
        if s == 1:
            for a in range(1, n):
                attn_scatter.start(a, attn[n - a])
        elif s < n - 1:
            attn_scatter.step(s, attn)
        experts([k for k in slots if k not in back])
    attn_scatter.step(n - 1, attn)

    half = n_groups * block // 2
    lines = []
    for h in range(2):
        part = slice(h * half, (h + 1) * half)
        pieces = [[(v, part) for v in back[k]] for k in range(n)]
        lines.append((LineScatter(n, seq), pieces))
    for s in range(1, n):
        for scatter, pieces in lines:
            scatter.start(s, pieces[n - s])
    for s in range(2, n):
        for scatter, pieces in lines:
            scatter.step(s, pieces)
    attn_output = seq.did(add_all(seq.after(*attn_scatter.finish(attn[0]))))
    home = []
    for h, (scatter, pieces) in enumerate(lines):
        addends = seq.after(*scatter.finish(pieces[0]))
        for k in range(n_groups // 2):
            values = []
            for v in addends:
                v, first = (v[0], v[1].start) if isinstance(v, tuple) else (v, 0)
                values.append((v, slice(first + k * block, first + (k + 1) * block)))
            part = seq.did(add_all(values))
            k += h * n_groups // 2
            home.append(around(part, k) if k else part)
    expert_output = combine(me, ids, home)
    return (attn_output, expert_output)


def solution(mesh):
    placed = (
        P("ep", "tp"),
        P("ep", "tp"),
        P("ep", "tp"),
        P("tp"),
        P("tp", None),
        P(("ep", "tp"), None),
        P(),
        P(("ep", "tp"), None),
        P(("ep", "tp"), None),
        P("ep", None, "tp"),
        P("ep", None, "tp"),
        P("ep", "tp", None),
    )
    return jax.shard_map(
        body,
        mesh=mesh,
        in_specs=placed,
        out_specs=(P(("ep", "tp"), None), P(("ep", "tp"), None)),
        check_vma=False,
    )
```

```python
import functools
import math

import jax
import jax.numpy as jnp
import numpy as np
from jax import lax
from jax.experimental import pallas as pl
from jax.experimental.pallas import tpu as pltpu
from jax.sharding import PartitionSpec as P


HD = 64
WINDOW = 128
EXP_DEV = 2
CORES = 2


theta_base = 10000.0
norm_eps = 1e-06
neg_large = -1e30
BF = jnp.bfloat16
F32 = jnp.float32


def gather_pairs(n, s, parity):
    pairs = []
    for link in range(parity, n - 1, 2):
        if link >= s - 1:
            pairs.append((link, link + 1))
        if link <= n - 1 - s:
            pairs.append((link + 1, link))
    return pairs


def scatter_pairs(n, s, parity):
    pairs = [(b, a) for a, b in gather_pairs(n, n - s, parity)]
    return [p for p in pairs if p not in first_hop(n)]


def first_hop(n):
    return [(0, 1), (n - 1, n - 2)]


def along(value, pairs):
    full = [(CORES * a + c, CORES * b + c) for a, b in pairs for c in range(CORES)]
    return lax.ppermute(value, "tp", full)


def core_swap(value):
    n = lax.axis_size("tp")
    return lax.ppermute(value, "tp", [(t, t ^ 1) for t in range(n)])


def slot_chunk(n, z, k):
    if k == 0:
        return z
    even = z % 2 == 0
    ec = jnp.where(even, n - 1 - z, z)
    o = n - k
    return jnp.where(
        k <= ec, jnp.where(even, z + k, z - k), jnp.where(even, z - o, z + o)
    )


def add_all(values):
    values = [v[0][v[1]] if isinstance(v, tuple) else v for v in values]
    if len(values) == 1:
        return values[0]
    return sum(v.astype(F32) for v in values).astype(BF)


class Sequence:
    def __init__(self):
        self.token = None

    def after(self, *values):
        arrays = [v[0] if isinstance(v, tuple) else v for v in values]
        arrays = lax.optimization_barrier((*arrays, self.token))[:-1]
        return [
            (a, v[1]) if isinstance(v, tuple) else a for a, v in zip(arrays, values)
        ]

    def did(self, value):
        self.token = value
        return value


class LineScatter:
    def __init__(self, n, seq):
        self.n = n
        self.seq = seq
        self.first = {}
        self.got = {}

    def send(self, values, pairs):
        values = self.seq.after(*values)
        out = add_all(values)
        if len(values) > 1:
            self.seq.did(out)
        return along(out, pairs)

    def start(self, s, slot):
        self.first[s] = self.send(slot, first_hop(self.n))

    def arrivals(self, s, parity):
        values = [self.got.get((s, parity))]
        if parity == 0:
            values.append(self.first.get(s))
        return [v for v in values if v is not None]

    def step(self, s, slots):
        for parity in (0, 1):
            pairs = scatter_pairs(self.n, s, parity)
            if pairs:
                slot = slots[self.n - s] if parity == 0 else slots[s]
                values = slot + self.arrivals(s - 1, 1 - parity)
                self.got[s, parity] = self.send(values, pairs)

    def finish(self, slot):
        last = self.n - 1
        return slot + self.arrivals(last, 0) + self.arrivals(last, 1)


def round_up(value, to):
    return -(-value // to) * to


def iota(shape, dim):
    return lax.broadcasted_iota(jnp.int32, shape, dim)


def routing(ids_ref, me_ref, block):
    ids = ids_ref[...].astype(F32)
    tokens = ids.shape[1]
    sq_row, sq_col = iota((tokens, tokens), 0), iota((tokens, tokens), 1)
    ids_col = jnp.sum(jnp.where(sq_row == sq_col, ids, 0.0), axis=1, keepdims=True)
    earlier = (ids_col == ids) & (sq_row < sq_col)
    rank = jnp.sum(earlier.astype(F32), axis=0, keepdims=True)
    group = (ids_ref[...] ^ me_ref[0]).astype(F32)
    slot = group * block + rank
    slot_col = jnp.sum(jnp.where(sq_row == sq_col, slot, 0.0), axis=1, keepdims=True)
    return group, rank, slot, slot_col


def tails_kernel(k_ref, v_ref, tail_ref):
    tail_ref[:WINDOW] = k_ref[...]
    tail_ref[WINDOW:] = v_ref[...]


def last_rows(keys, values):
    rows, narrow = keys.shape
    last = pl.BlockSpec((WINDOW, narrow), lambda i: (rows // WINDOW - 1, 0))
    return pl.pallas_call(
        tails_kernel,
        grid=(1,),
        in_specs=[last, last],
        out_specs=pl.BlockSpec((2 * WINDOW, narrow), lambda i: (0, 0)),
        out_shape=jax.ShapeDtypeStruct((2 * WINDOW, narrow), BF),
        compiler_params=pltpu.CompilerParams(vmem_limit_bytes=60 << 20),
        name="last_rows",
    )(keys, values)


def dispatch_kernel(capacity, block, count, me_ref, x_ref, gain_ref, ids_ref, share_ref, *refs):
    sources, sems = refs[:count], refs[-1]
    out_refs, held = refs[count : -1 - count], refs[-1 - count : -1]
    copies = [
        pltpu.make_async_copy(a, b, sems.at[i]) for i, (a, b) in enumerate(zip(sources, held))
    ]
    for copy in copies:
        copy.start()
    rows = len(out_refs) * block
    tokens = x_ref.shape[0]
    lanes = 128
    x = x_ref[...].astype(F32)
    scale = lax.rsqrt(jnp.mean(x * x, axis=-1, keepdims=True) + norm_eps)
    normed = (x * scale * gain_ref[...]).astype(BF)
    group, rank, slot, _ = routing(ids_ref, me_ref, block)
    row_id = iota((rows, tokens), 0)
    picker = (row_id.astype(F32) == slot).astype(BF)
    out = jnp.dot(picker, normed, preferred_element_type=F32)
    place = row_id % block - capacity
    same = (row_id // block).astype(F32) == group
    weight = jnp.zeros((rows, tokens), F32)
    for k in range(EXP_DEV):
        share = share_ref[k : k + 1, :].astype(BF).astype(F32)
        weight = jnp.where(same & (place == k), share, weight)
    sq_row, sq_col = iota((tokens, tokens), 0), iota((tokens, tokens), 1)
    rank_col = jnp.sum(jnp.where(sq_row == sq_col, rank, 0.0), axis=1, keepdims=True)
    by_rank = (rank_col == iota((tokens, lanes), 1).astype(F32)).astype(BF)
    tail = jnp.dot(weight.astype(BF), by_rank, preferred_element_type=F32)
    for g, out_ref in enumerate(out_refs):
        part = slice(g * block, (g + 1) * block)
        out_ref[:, :lanes] = (out[part, :lanes] + tail[part]).astype(BF)
        out_ref[:, lanes:] = out[part, lanes:].astype(BF)
    for copy in copies:
        copy.wait()


def in_vmem(count):
    return [pl.BlockSpec(memory_space=pltpu.VMEM)] * count


def dispatch(me, x, gain, ids, share, n_groups, capacity, block, keep):
    gain = gain.reshape(1, -1)

    def whole(shape):
        return pl.BlockSpec(shape, lambda i: (0, 0))

    outs = [(block, x.shape[1])] * n_groups
    return pl.pallas_call(
        functools.partial(dispatch_kernel, capacity, block, len(keep)),
        grid=(1,),
        in_specs=[pl.BlockSpec(memory_space=pltpu.SMEM)]
        + [whole(v.shape) for v in (x, gain, ids, share)]
        + [pl.BlockSpec(memory_space=pltpu.HBM)] * len(keep),
        out_specs=[whole(o) for o in outs] + in_vmem(len(keep)),
        out_shape=[jax.ShapeDtypeStruct(o, BF) for o in outs]
        + [pltpu.VMEM(v.shape, v.dtype) for v in keep],
        scratch_shapes=[pltpu.SemaphoreType.DMA((len(keep),))],
        compiler_params=pltpu.CompilerParams(vmem_limit_bytes=61 << 20),
        name="dispatch",
    )(me, x, gain, ids, share, *keep)


def pack_kernel(*refs):
    *parts, out_ref = refs
    block = parts[0].shape[0]
    for i, part in enumerate(parts):
        out_ref[i * block : (i + 1) * block] = part[...]


def pack(parts):
    block, width = parts[0].shape
    return pl.pallas_call(
        pack_kernel,
        in_specs=in_vmem(len(parts)),
        out_specs=in_vmem(1)[0],
        out_shape=jax.ShapeDtypeStruct((len(parts) * block, width), BF),
        compiler_params=pltpu.CompilerParams(vmem_limit_bytes=16 << 20),
        name="pack",
    )(*parts)


def combine_kernel(block, me_ref, ids_ref, *refs):
    *parts, out_ref = refs
    tokens = out_ref.shape[0]
    slot_col = routing(ids_ref, me_ref, block)[3]
    rows = jnp.concatenate([p[...] for p in parts], axis=0)
    picker = (slot_col == iota((tokens, rows.shape[0]), 1).astype(F32)).astype(BF)
    out_ref[...] = jnp.dot(picker, rows, preferred_element_type=F32).astype(BF)


def combine(me, ids, parts):
    block, width = parts[0].shape
    return pl.pallas_call(
        functools.partial(combine_kernel, block),
        in_specs=[pl.BlockSpec(memory_space=pltpu.SMEM)] + in_vmem(1 + len(parts)),
        out_shape=jax.ShapeDtypeStruct((ids.shape[1], width), BF),
        compiler_params=pltpu.CompilerParams(vmem_limit_bytes=16 << 20),
        name="combine",
    )(me, ids, *parts)


def expert_kernel(capacity, block, count, *refs):
    parts, refs = refs[:count], refs[count:]
    gate_ref, up_ref, down_ref = refs[:3]
    outs = refs[3 : 3 + count]
    x_s, h_s = refs[3 + count :]
    half = parts[0].shape[0]
    units = gate_ref.shape[2]
    for i, part in enumerate(parts):
        x_s[i * half : (i + 1) * half] = part[...]
    row, col = iota((half, half), 0), iota((half, half), 1)
    mine = iota((half, 128), 0) % block == iota((half, 128), 1)
    shares = []
    for k in range(EXP_DEV):
        take = (col == row - row % block + capacity + k).astype(BF)
        columns = []
        for part in parts:
            spread = jnp.dot(take, part[:, :128], preferred_element_type=F32)
            columns.append(jnp.sum(jnp.where(mine, spread, 0.0), axis=1, keepdims=True))
        shares.append(jnp.concatenate(columns, axis=0))
    cut = math.gcd(units, 256)
    for k in range(EXP_DEV):
        for c in range(0, units, cut):
            x = x_s[...]
            gate = jnp.dot(x, gate_ref[k, :, c : c + cut], preferred_element_type=F32)
            up = jnp.dot(x, up_ref[k, :, c : c + cut], preferred_element_type=F32)
            hidden = gate / (1.0 + jnp.exp(-gate)) * up * shares[k]
            h_s[:, k * units + c : k * units + c + cut] = hidden.astype(BF)
    width = x_s.shape[1]
    piece = math.gcd(width, 512)
    for c in range(0, width, piece):
        total = jnp.dot(h_s[...], down_ref[:, c : c + piece], preferred_element_type=F32)
        for i, out in enumerate(outs):
            out[:, c : c + piece] = total[i * half : (i + 1) * half].astype(BF)


def expert_rows(parts, gate, up, down, capacity, block):
    count = len(parts)
    half, width = parts[0].shape
    units = gate.shape[2]
    return pl.pallas_call(
        functools.partial(expert_kernel, capacity, block, count),
        in_specs=in_vmem(count + 3),
        out_specs=in_vmem(count),
        out_shape=[jax.ShapeDtypeStruct((half, width), BF)] * count,
        scratch_shapes=[
            pltpu.VMEM((count * half, width), BF),
            pltpu.VMEM((count * half, EXP_DEV * units), BF),
        ],
        cost_estimate=pl.CostEstimate(
            flops=2 * count * half * width * units * EXP_DEV * 3,
            bytes_accessed=4 * count * half * width,
            transcendentals=count * half * units * EXP_DEV,
        ),
        compiler_params=pltpu.CompilerParams(vmem_limit_bytes=24 << 20),
        name="experts",
    )(*parts, gate, up, down)


def attention_kernel(
    kv_here,
    per_group,
    many,
    order_ref,
    base_ref,
    sink_ref,
    q_ref,
    k_ref,
    v_ref,
    tail_ref,
    step_ref,
    start_ref,
    turn_ref,
    w_ref,
    *rest,
):
    span = WINDOW
    turn = turn_ref[...]
    plus_ref = rest[0] if len(rest) > 1 else None
    outs = rest[1:]
    step = pl.program_id(0)
    shape = (per_group * span, 2 * span)
    row = lax.broadcasted_iota(jnp.int32, shape, 0)
    col = lax.broadcasted_iota(jnp.int32, shape, 1)
    lag = row % span + span - col
    inside = (lag >= 0) & (lag < span)
    column = lax.broadcasted_iota(jnp.int32, (per_group * span, 1), 0) // span
    sinks = []
    for c in range(kv_here):
        sink = jnp.full((per_group * span, 1), sink_ref[c * per_group], F32)
        for g in range(1, per_group):
            sink = jnp.where(column == g, sink_ref[c * per_group + g], sink)
        sinks.append(sink)

    def rotated(x, at, scale):
        width = x.shape[1]
        cos_i, sin_i = step_ref[0, :, :width], step_ref[1, :, :width]
        base = start_ref[at]
        cos_0, sin_0 = base[0:1, :width], base[1:2, :width]
        cosine = cos_0 * cos_i - sin_0 * sin_i
        sine = sin_0 * cos_i + cos_0 * sin_i
        swapped = jnp.dot(x, turn[:width, :width], preferred_element_type=F32)
        return ((x.astype(F32) * cosine + swapped * sine) * scale).astype(BF)

    for b in range(many):
        index = order_ref[step * many + b]
        first = index == 0
        place = base_ref[0] + index
        here = pl.ds(pl.multiple_of(index * span, span), span)
        back = pl.ds(pl.multiple_of(jnp.maximum(index - 1, 0) * span, span), span)
        q = rotated(q_ref[here, :], place, 1.0 / math.sqrt(HD))
        before_k = jnp.where(first, tail_ref[:span], k_ref[back, :])
        before_v = jnp.where(first, tail_ref[span:], v_ref[back, :])
        keys = jnp.concatenate(
            [
                rotated(before_k, jnp.maximum(place - 1, 0), 1.0),
                rotated(k_ref[here, :], place, 1.0),
            ],
            axis=0,
        )
        values = jnp.concatenate([before_v, v_ref[here, :]], axis=0)
        allowed = inside & (col >= jnp.where(place == 0, span, 0))
        attended = []
        for c in range(kv_here):
            heads = [c * per_group + g for g in range(per_group)]
            rows = jnp.concatenate([q[:, h * HD : (h + 1) * HD] for h in heads], axis=0)
            key = keys[:, c * HD : (c + 1) * HD]
            scores = lax.dot_general(
                rows, key, (((1,), (1,)), ((), ())), preferred_element_type=F32
            )
            scores = jnp.where(allowed, scores, neg_large)
            top = jnp.maximum(jnp.max(scores, axis=1, keepdims=True), sinks[c])
            expo = jnp.exp(scores - top)
            denom = jnp.sum(expo, axis=1, keepdims=True) + jnp.exp(sinks[c] - top)
            mixed = jnp.dot(
                expo.astype(BF), values[:, c * HD : (c + 1) * HD], preferred_element_type=F32
            )
            mixed = (mixed / denom).astype(BF)
            attended += [mixed[g * span : (g + 1) * span] for g in range(per_group)]
        attended = jnp.concatenate(attended, axis=1)
        total = jnp.dot(attended, w_ref[...], preferred_element_type=F32)
        if plus_ref is None:
            rest[0][b] = total.astype(BF)
            continue
        total = (total + plus_ref[b].astype(F32)).astype(BF)
        for i in range(b, len(outs), many):

            @pl.when(step == i // many)
            def _(i=i):
                outs[i][...] = total


def rotary_tables(width, blocks):
    half = HD // 2
    frequency = theta_base ** (-(np.arange(half, dtype=np.float64) * 2.0) / HD)
    lanes = np.tile(frequency, width // half)[None, :]
    inside = np.arange(WINDOW)[:, None] * lanes
    starts = (np.arange(blocks) * WINDOW)[:, None] * lanes
    steps = np.stack([np.cos(inside), np.sin(inside)]).astype(np.float32)
    bases = np.stack([np.cos(starts), np.sin(starts)], axis=1).astype(np.float32)
    lane = np.arange(width)
    turn = np.zeros((width, width), np.float32)
    low = lane % HD < half
    turn[np.where(low, lane + half, lane - half), lane] = np.where(low, -1.0, 1.0)
    return steps, bases, turn


def attention_partials(
    order, base, queries, keys, values, tails, sinks, weight, tables, plus=None
):
    width = queries.shape[1]
    narrow = keys.shape[1]
    kv_here = narrow // HD
    per_group = width // narrow
    count = order.shape[0]
    many = count
    operands = (
        queries,
        keys,
        values,
        tails,
        *tables,
        weight,
    )

    def fixed(x):
        return pl.BlockSpec(x.shape, lambda i, o, b, s: (0,) * len(x.shape))

    out_width = weight.shape[1]
    stack = pl.BlockSpec((many, WINDOW, out_width), lambda i, o, b, s: (i, 0, 0))
    in_specs = in_vmem(3) + [fixed(tails)] + in_vmem(4)
    if plus is None:
        out_specs, out_shape = stack, jax.ShapeDtypeStruct((count, WINDOW, out_width), BF)
    else:
        operands += (plus,)
        in_specs += [stack]
        out_shape = [jax.ShapeDtypeStruct((WINDOW, out_width), BF)] * count
        out_specs = [fixed(o) for o in out_shape]
    return pl.pallas_call(
        functools.partial(attention_kernel, kv_here, per_group, many),
        grid_spec=pltpu.PrefetchScalarGridSpec(
            num_scalar_prefetch=3,
            grid=(count // many,),
            in_specs=in_specs,
            out_specs=out_specs,
        ),
        out_shape=out_shape,
        cost_estimate=pl.CostEstimate(
            flops=16 * count * WINDOW * width * (weight.shape[1] + 4 * WINDOW),
            bytes_accessed=2 * weight.size + 2 * count * WINDOW * (weight.shape[1] + 2 * width),
            transcendentals=count * WINDOW * 2 * WINDOW * kv_here * per_group,
        ),
        compiler_params=pltpu.CompilerParams(vmem_limit_bytes=28 << 20),
        name="attention",
    )(order, base, sinks, *operands)


def body(
    queries,
    key_rows,
    value_rows,
    sink_logits,
    out_weight,
    expert_input,
    norm_gain,
    group_ids,
    route_weight,
    gate_weight,
    up_weight,
    down_weight,
):
    n_groups = lax.axis_size("ep")
    n_tp = lax.axis_size("tp")
    n = n_tp // CORES
    token_count, width = expert_input.shape
    capacity = max(2, token_count * 5 // (4 * n_groups))
    block = round_up(capacity + EXP_DEV, 8)
    e = lax.axis_index("ep")
    t = lax.axis_index("tp")
    z, core = t // CORES, t % CORES
    me = e.reshape(1)
    ids = group_ids.reshape(1, token_count)
    seq = Sequence()

    def around(part, k):
        return lax.ppermute(part, "ep", [(i, i ^ k) for i in range(n_groups)])

    tails = seq.did(last_rows(key_rows, value_rows))
    before = lax.ppermute(tails, "ep", [(i, i + 1) for i in range(n_groups - 1)])
    (x,) = seq.after(expert_input)
    tables = rotary_tables(queries.shape[1], n_groups * n_tp)
    tables = [jnp.asarray(v, d) for v, d in zip(tables, (F32, F32, BF))]
    keep = (queries, key_rows, value_rows, out_weight, *tables)
    done = dispatch(me, x, norm_gain, ids, route_weight.T, n_groups, capacity, block, keep)
    send, (queries, key_rows, value_rows, out_weight, *tables) = done[:n_groups], done[n_groups:]
    seq.did(send[0])
    got = [send[0]] + [around(send[k], k) for k in range(1, n_groups)]

    chunk = jnp.stack([slot_chunk(n, z, k) for k in range(n)]) * CORES

    def attend(order, plus=None):
        q = queries
        (order,) = seq.after(order)
        return attention_partials(
            order,
            (e * n_tp).reshape(1),
            q,
            key_rows,
            value_rows,
            before,
            sink_logits,
            out_weight,
            tables,
            plus,
        )

    arrived = {}

    def gather(s):
        for parity in (1, 0):
            pairs = gather_pairs(n, s, parity)
            if pairs:
                value = own
                if s > 1:
                    (value,) = seq.after(arrived[s - 1, 1 - parity])
                arrived[s, parity] = along(value, pairs)

    slots = {}

    def prepare(s):
        for k in range(1, n):
            late = n - k if gather_pairs(n, n - k, 1) else 0
            if max(k, late) == s:
                addends = [arrived[k, 0], arrived.get((n - k, 1))]
                slot = add_all([a for a in addends if a is not None])
                slots[k] = [slot, core_swap(slot)]

    back = {}

    def experts(ks):
        for k in ks:
            parts = seq.after(*slots[k])
            done = expert_rows(parts, *weights, capacity, block)
            seq.did(done[0])
            back[k] = [done[0], core_swap(done[1])]

    other = seq.did(attend(chunk + 1 - core))
    swapped = core_swap(other)
    weights = seq.after(gate_weight, up_weight, down_weight.reshape(-1, width))
    own = seq.did(pack(seq.after(*got)))
    gather(1)
    slots[0] = [own, core_swap(own)]
    (swapped,) = seq.after(swapped)
    mine = attend(chunk + core, swapped)
    seq.did(mine[0])
    attn = [[v] for v in mine]
    attn_scatter = LineScatter(n, seq)
    for s in range(1, n):
        attn_scatter.start(s, attn[n - s])
    for s in range(1, n):
        if s < n - 1:
            gather(s + 1)
        if s > 1:
            attn_scatter.step(s, attn)
        prepare(s)
        experts([k for k in slots if k not in back])
    half = n_groups * block // 2
    lines = []
    for h in range(2):
        part = slice(h * half, (h + 1) * half)
        pieces = [[(v, part) for v in back[k]] for k in range(n)]
        lines.append((LineScatter(n, seq), pieces))
    for s in range(1, n):
        for scatter, pieces in lines:
            scatter.start(s, pieces[n - s])
    for s in range(2, n):
        for scatter, pieces in lines:
            scatter.step(s, pieces)
    attn_output = seq.did(add_all(seq.after(*attn_scatter.finish(attn[0]))))
    home = []
    for h, (scatter, pieces) in enumerate(lines):
        addends = seq.after(*scatter.finish(pieces[0]))
        for k in range(n_groups // 2):
            values = []
            for v in addends:
                v, first = (v[0], v[1].start) if isinstance(v, tuple) else (v, 0)
                values.append((v, slice(first + k * block, first + (k + 1) * block)))
            part = seq.did(add_all(values))
            k += h * n_groups // 2
            home.append(around(part, k) if k else part)
    expert_output = combine(me, ids, home)
    return (attn_output, expert_output)


def solution(mesh):
    placed = (
        P("ep", "tp"),
        P("ep", "tp"),
        P("ep", "tp"),
        P("tp"),
        P("tp", None),
        P(("ep", "tp"), None),
        P(),
        P(("ep", "tp"), None),
        P(("ep", "tp"), None),
        P("ep", None, "tp"),
        P("ep", None, "tp"),
        P("ep", "tp", None),
    )
    return jax.shard_map(
        body,
        mesh=mesh,
        in_specs=placed,
        out_specs=(P(("ep", "tp"), None), P(("ep", "tp"), None)),
        check_vma=False,
    )
```
